32 devices in a mesh: ep: 16 (over z, y, x), tp: 2 (over core).
Axes of the slice: x: 2, y: 2, z: 4, core: 2. Of those that a mesh axis runs over, the one named last changes fastest.
Arguments:
- resid: bfloat16 [256, 2048], P('ep'), may hold values from -6 to 6
- proj_x: bfloat16 [256, 2048], P('ep', 'tp'), may hold values from -6 to 6
- proj_z: bfloat16 [256, 2048], P('ep', 'tp'), may hold values from -6 to 6
- proj_bc: bfloat16 [256, 2, 512], P('ep', None, 'tp'), may hold values from -6 to 6
- proj_dt: bfloat16 [256, 32], P('ep', 'tp'), may hold values from -6 to 6
- tail_x: bfloat16 [256, 3, 2048], P('ep', None, 'tp'), may hold values from -6 to 6
- tail_bc: bfloat16 [256, 3, 2, 512], P('ep', None, None, 'tp'), may hold values from -6 to 6
- taps_x: bfloat16 [4, 2048], P(None, 'tp'), may hold values from -3 to 3
- taps_bc: bfloat16 [4, 2, 512], P(None, None, 'tp'), may hold values from -3 to 3
- ssm_state: float32 [256, 32, 4096], P('ep', 'tp'), may hold values from -1.5 to 1.5
- dt_bias: float32 [32], P('tp'), may hold values from -4 to 0
- decay_log: float32 [32], P('tp'), may hold values from -1 to 2.5
- group_gain: float32 [2048], P('tp'), may hold values from 0.1 to 1.9
- out_proj: bfloat16 [2048, 2048], P('tp', 'ep'), may hold values from -0.125 to 0.125
- ffn_gain: float32 [2048], replicated, may hold values from 0.1 to 1.9
- dense_gate: bfloat16 [2048, 4096], P(None, ('ep', 'tp')), may hold values from -0.125 to 0.125
- dense_up: bfloat16 [2048, 4096], P(None, ('ep', 'tp')), may hold values from -0.125 to 0.125
- dense_down: bfloat16 [4096, 2048], P(('ep', 'tp')), may hold values from -0.09375 to 0.09375
- branch_gate: bfloat16 [2048], replicated, may hold values from -0.125 to 0.125
- group_weights: float32 [256, 4], replicated, may hold values from 0.2 to 1
- expert_ids: int32 [256, 6], replicated, may hold values from 0 to 15, all different within a row; in each aligned block of 16 rows (0 to 15, 16 to 31, ...) at most 7 rows name the same one
- expert_weights: float32 [256, 6], replicated, may hold values from 0.1 to 1
- exp_gate: bfloat16 [16, 2048, 512], P('ep', None, 'tp'), may hold values from -0.125 to 0.125
- exp_up: bfloat16 [16, 2048, 512], P('ep', None, 'tp'), may hold values from -0.125 to 0.125
- exp_down: bfloat16 [16, 512, 2048], P('ep', 'tp'), may hold values from -0.25 to 0.25
Outputs:
- out: bfloat16 [256, 2048], P(('ep', 'tp'))
- new_state: float32 [256, 32, 4096], P('ep', 'tp')
The draws below stay inside these ranges and needn't reach their ends.
Inputs may be any that keep to these rules, and one draw needn't show every extreme that they name: `expert_ids`: each row names 6 different experts. In the rows of one index of ep (aligned blocks of 16 rows) no expert is named more than 7 times, a bound that some block reaches.
All inputs are finite; a program needn't handle non-finite values.
Results may differ from the reference program's by a relative error of at most 0.013.
Values may be sent and summed in bfloat16 or wider, within the bound.
No kernel may reach another device: no remote copies, remote signals or barrier semaphores. Data moves between devices by JAX's collectives and lax.ppermute only.
A program may use at most 128 MiB of HBM per device.

```python
import math
import jax
import jax.numpy as jnp
import numpy as np
from jax import lax

D = 2048
HEADS = 32
HEAD_P = 64
NSTATE = 64
BC_GROUPS = 8
TAPS = 4
EFF = 512
DFF = 4096
GROUPS = 4
TOPK = 6
SEQ_DEV = 16
INNER = 2048
HPG = 4
BATCH = 256
EXPERTS = 16
EPG = 4
CAP = 7


def block_scale(own_key, dims, shards, smallest, largest):
    gain, own = 1.0, jax.random.fold_in(own_key, 6)
    for dim, parts in shards:
        steps = jnp.exp(jax.random.uniform(jax.random.fold_in(own, dim), (parts,), jnp.float32, smallest / len(shards), largest / len(shards)))
        gain = gain * jnp.repeat(steps, dims[dim] // parts).reshape([-1 if axis == dim else 1 for axis in range(len(dims))])
    return gain


def shared_out(own_key, own, number, rows, count, top, most, slope):
    sequence = jax.random.permutation(own_key, count)
    crowded, common = portions_of(count, rows * top, most, slope, True), portions_of(count, rows * top, most, slope, False)
    places = jnp.arange(count)

    def named(lengths, offset_by):
        used = int((lengths > 0).sum())
        fixed = max(1, used // 4)
        shifted = fixed + (places - fixed + offset_by * (used - fixed)) % max(1, count - fixed)
        return jnp.zeros((count,), jnp.int32).at[sequence[jnp.where(places < fixed, places, shifted)]].set(jnp.asarray(lengths, jnp.int32))

    lengths = jnp.where(number % 4 == 0, named(crowded, number // 4), named(common, number - number // 4 - 1))
    mixed = jax.random.permutation(jax.random.fold_in(own, 3), count)
    donor, receiver = mixed[0:count // 2 * 2:2], mixed[1:count // 2 * 2:2]
    room = jnp.minimum(lengths[donor] - 1, most - lengths[receiver]) // 2
    room = jnp.where((donor == sequence[0]) | (receiver == sequence[0]) | (lengths[receiver] == 0), 0, jnp.maximum(room, 0))
    shifted = jax.random.randint(jax.random.fold_in(own, 4), (count // 2,), 0, 1 << 20) % (room + 1)
    lengths = lengths.at[donor].add(-shifted).at[receiver].add(shifted)
    members = jnp.searchsorted(jnp.cumsum(lengths), jnp.arange(rows * top), side="right").astype(jnp.int32)
    table = members.reshape(top, rows).T
    table = table[jax.random.permutation(jax.random.fold_in(own, 1), rows)]
    offset_by = jax.random.randint(jax.random.fold_in(own, 2), (rows, 1), 0, top)
    return jnp.take_along_axis(table, (jnp.arange(top)[None, :] + offset_by) % top, axis=1)


def portions_of(count, total, limit, lean, full):
    loads = [(1 << 20) // math.isqrt(standing ** lean) + 1 for standing in range(1, count + 1)]
    largest = limit if full else min(limit, max(-(-total // count), total * loads[0] // sum(loads)))
    least = 1 if total - largest >= count - 1 else 0
    holding, rest = [largest] + [least] * (count - 1), total - largest - least * (count - 1)
    while rest > 0:
        free = [i for i in range(1, count) if holding[i] < largest] or [i for i in range(1, count) if holding[i] < limit]
        whole, left = sum([loads[i] for i in free]), rest
        for i in free:
            addition = min(limit - holding[i], max(1, left * loads[i] // whole), rest)
            holding[i] = holding[i] + addition
            rest = rest - addition
    return np.array(holding)


def gaussian(stream_key, dims, scale, most, cuts=(), kind=jnp.bfloat16):
    drawn = jax.random.normal(stream_key, dims, jnp.float32) * scale
    if len(cuts) > 0:
        drawn = block_scale(stream_key, dims, cuts, -0.22, 0.18) * drawn
    return jnp.clip(drawn, min=-most, max=most).astype(kind)


def setup_inputs(seed: int = 0) -> dict:
    key_of = jax.random.split(jax.random.key(seed), 26)
    resid = gaussian(key_of[0], (BATCH, D), 1.0, 6.0, ((0, 16),))
    proj_x = gaussian(key_of[1], (BATCH, INNER), 1.0, 6.0, ((0, 16), (1, 2)))
    proj_z = gaussian(key_of[2], (BATCH, INNER), 1.0, 6.0, ((0, 16), (1, 2)))
    proj_bc = gaussian(key_of[3], (BATCH, 2, BC_GROUPS * NSTATE), 1.0, 6.0, ((0, 16), (2, 2)))
    proj_dt = gaussian(key_of[4], (BATCH, HEADS), 1.0, 6.0, ((0, 16), (1, 2)))
    tail_x = gaussian(key_of[5], (BATCH, TAPS - 1, INNER), 1.0, 6.0, ((0, 16), (2, 2)))
    tail_bc = gaussian(key_of[6], (BATCH, TAPS - 1, 2, BC_GROUPS * NSTATE), 1.0, 6.0, ((0, 16), (3, 2)))
    taps_x = gaussian(key_of[7], (TAPS, INNER), TAPS ** -0.5, 3.0, ((1, 2),))
    taps_bc = gaussian(key_of[8], (TAPS, 2, BC_GROUPS * NSTATE), TAPS ** -0.5, 3.0, ((2, 2),))
    ssm_state = gaussian(key_of[9], (BATCH, HEADS, HEAD_P * NSTATE), 0.25, 1.5, ((0, 16), (1, 2)), jnp.float32)
    dt_bias = jnp.clip(-4.0 + 4.0 * jax.random.uniform(key_of[10], (HEADS,), jnp.float32) ** block_scale(key_of[10], (HEADS,), ((0, 2),), -0.2, 0.2), -4.0, 0.0)
    decay_log = jnp.clip(-1.0 + 3.5 * jax.random.uniform(key_of[11], (HEADS,), jnp.float32) ** block_scale(key_of[11], (HEADS,), ((0, 2),), -0.2, 0.2), -1.0, 2.5)
    group_gain = jnp.clip(1.0 + 0.18 * jax.random.normal(key_of[12], (INNER,), jnp.float32), 0.1, 1.9)
    out_proj = gaussian(key_of[13], (INNER, D), INNER ** -0.5, 0.125, ((0, 2), (1, 16)))
    ffn_gain = jnp.clip(1.0 + 0.18 * jax.random.normal(key_of[14], (D,), jnp.float32), 0.1, 1.9)
    dense_gate = gaussian(key_of[15], (D, DFF), D ** -0.5, 0.125, ((1, 32),))
    dense_up = gaussian(key_of[16], (D, DFF), D ** -0.5, 0.125, ((1, 32),))
    dense_down = gaussian(key_of[17], (DFF, D), DFF ** -0.5, 0.09375, ((0, 32),))
    branch_gate = gaussian(key_of[18], (D,), D ** -0.5, 0.125)
    group_weights = jnp.clip(jnp.exp(jax.random.uniform(key_of[19], (BATCH, GROUPS), jnp.float32, math.log(0.2), math.log(1.0))), 0.2, 1.0)
    expert_ids_keys = jax.random.split(jax.random.fold_in(key_of[20], 1), BATCH // SEQ_DEV)
    expert_ids_turns = jax.random.permutation(jax.random.fold_in(key_of[20], 3), BATCH // SEQ_DEV)
    expert_ids = jax.vmap(lambda own, number: shared_out(jax.random.fold_in(key_of[20], 2), own, number, SEQ_DEV, EXPERTS, TOPK, CAP, 2))(expert_ids_keys, expert_ids_turns).reshape((BATCH, TOPK))
    expert_weights = jnp.clip(jnp.exp(jax.random.uniform(key_of[21], (BATCH, TOPK), jnp.float32, math.log(0.1), math.log(1.0))), 0.1, 1.0)
    exp_gate = gaussian(key_of[22], (EXPERTS, D, EFF), D ** -0.5, 0.125, ((0, 16), (2, 2)))
    exp_up = gaussian(key_of[23], (EXPERTS, D, EFF), D ** -0.5, 0.125, ((0, 16), (2, 2)))
    exp_down = gaussian(key_of[24], (EXPERTS, EFF, D), EFF ** -0.5, 0.25, ((0, 16), (1, 2)))
    return {"resid": resid, "proj_x": proj_x, "proj_z": proj_z, "proj_bc": proj_bc, "proj_dt": proj_dt, "tail_x": tail_x, "tail_bc": tail_bc, "taps_x": taps_x, "taps_bc": taps_bc, "ssm_state": ssm_state, "dt_bias": dt_bias, "decay_log": decay_log, "group_gain": group_gain, "out_proj": out_proj, "ffn_gain": ffn_gain, "dense_gate": dense_gate, "dense_up": dense_up, "dense_down": dense_down, "branch_gate": branch_gate, "group_weights": group_weights, "expert_ids": expert_ids, "expert_weights": expert_weights, "exp_gate": exp_gate, "exp_up": exp_up, "exp_down": exp_down}


EPSILON = 1e-06

def state_update(proj_x, proj_z, proj_bc, proj_dt, tail_x, tail_bc, taps_x, taps_bc, ssm_state, dt_bias, decay_log, group_gain):
    window_x = jnp.concatenate([tail_x, proj_x[:, None]], axis=1).astype(jnp.float32)
    conv_x = jax.nn.silu(lax.optimization_barrier(jnp.sum(window_x * taps_x.astype(jnp.float32)[None], axis=1)))
    window_bc = jnp.concatenate([tail_bc, proj_bc[:, None]], axis=1).astype(jnp.float32)
    conv_bc = jax.nn.silu(lax.optimization_barrier(jnp.sum(window_bc * taps_bc.astype(jnp.float32)[None], axis=1)))
    count = proj_x.shape[0]
    heads = proj_dt.shape[1]
    x_heads = conv_x.reshape(count, heads, HEAD_P)
    grouped_bc = conv_bc.reshape(count, 2, heads // HPG, NSTATE)
    input_heads = jnp.repeat(grouped_bc[:, 0], HPG, axis=1)
    read_heads = jnp.repeat(grouped_bc[:, 1], HPG, axis=1)
    step_size = jax.nn.softplus(proj_dt.astype(jnp.float32) + dt_bias)
    decay = jnp.exp(-step_size * jnp.exp(decay_log))
    state = ssm_state.reshape(count, heads, HEAD_P, NSTATE)
    fresh = (step_size[:, :, None] * x_heads)[:, :, :, None] * input_heads[:, :, None, :]
    new_state = decay[:, :, None, None] * state + fresh
    readout = lax.optimization_barrier(jnp.sum(new_state * read_heads[:, :, None, :], axis=-1))
    gated = readout.reshape(count, heads * HEAD_P) * jax.nn.silu(proj_z.astype(jnp.float32))
    grouped = gated.reshape(count, heads // HPG, HPG * HEAD_P)
    grouped = grouped * lax.rsqrt(lax.optimization_barrier(jnp.mean(grouped * grouped, axis=-1, keepdims=True)) + EPSILON)
    y_out = (grouped.reshape(count, heads * HEAD_P) * group_gain).astype(jnp.bfloat16)
    return (y_out, new_state.reshape(count, heads, HEAD_P * NSTATE))

def expert_slots(expert_ids, expert_weights, group_weights, index, experts, group_size, capacity):
    batch = expert_ids.shape[0]
    rows_each = batch // experts
    pairs = rows_each * TOPK
    pick = (jnp.arange(GROUPS, dtype=jnp.int32) == index // group_size).astype(jnp.float32)
    coarse = lax.optimization_barrier(jnp.sum(group_weights * pick[None], axis=1))
    pair_weight = (expert_weights * coarse[:, None]).reshape(experts, pairs)
    hits = (expert_ids.reshape(experts, pairs) == index).astype(jnp.int32)
    ranks = jnp.cumsum(hits, axis=1, dtype=jnp.int32)
    levels = jnp.arange(1, capacity + 1, dtype=jnp.int32)
    select = hits[:, None, :] * (ranks[:, None, :] == levels[None, :, None]).astype(jnp.int32)
    pair_row = jnp.arange(pairs, dtype=jnp.int32) // TOPK
    local_row = lax.optimization_barrier(jnp.sum(select * pair_row[None, None, :], axis=-1, dtype=jnp.int32))
    filled = lax.optimization_barrier(jnp.sum(select, axis=-1, dtype=jnp.int32)).reshape(-1)
    slot_weight = lax.optimization_barrier(jnp.sum(select.astype(jnp.float32) * pair_weight[:, None, :], axis=-1)).reshape(-1)
    row_index = (local_row + jnp.arange(experts, dtype=jnp.int32)[:, None] * rows_each).reshape(-1)
    return (row_index, filled, slot_weight)

def reference(resid, proj_x, proj_z, proj_bc, proj_dt, tail_x, tail_bc, taps_x, taps_bc, ssm_state, dt_bias, decay_log, group_gain, out_proj, ffn_gain, dense_gate, dense_up, dense_down, branch_gate, group_weights, expert_ids, expert_weights, exp_gate, exp_up, exp_down):
    y_out, new_state = state_update(proj_x, proj_z, proj_bc, proj_dt, tail_x, tail_bc, taps_x, taps_bc, ssm_state, dt_bias, decay_log, group_gain)
    mixed = jnp.dot(y_out, out_proj, preferred_element_type=jnp.float32)
    resid_new = (resid.astype(jnp.float32) + mixed).astype(jnp.bfloat16)
    widened = resid_new.astype(jnp.float32)
    normed = (widened * lax.rsqrt(lax.optimization_barrier(jnp.mean(widened * widened, axis=-1, keepdims=True)) + EPSILON) * ffn_gain).astype(jnp.bfloat16)
    score = jnp.dot(normed, branch_gate, preferred_element_type=jnp.float32)
    dense_pre = jnp.dot(normed, dense_gate, preferred_element_type=jnp.float32)
    dense_lin = jnp.dot(normed, dense_up, preferred_element_type=jnp.float32)
    dense_hidden = (jax.nn.sigmoid(score)[:, None] * jax.nn.silu(dense_pre) * dense_lin).astype(jnp.bfloat16)
    total = jnp.dot(dense_hidden, dense_down, preferred_element_type=jnp.float32)

    def expert_step(accum, items):
        gate_w, up_w, down_w, index = items
        row_index, filled, slot_weight = expert_slots(expert_ids, expert_weights, group_weights, index, EXPERTS, EPG, CAP)
        slot_rows = jnp.take(normed, row_index, axis=0)
        slot_pre = jnp.dot(slot_rows, gate_w, preferred_element_type=jnp.float32)
        slot_lin = jnp.dot(slot_rows, up_w, preferred_element_type=jnp.float32)
        slot_hidden = (slot_weight[:, None] * jax.nn.silu(slot_pre) * slot_lin).astype(jnp.bfloat16)
        slot_out = jnp.dot(slot_hidden, down_w, preferred_element_type=jnp.float32)
        slot_out = slot_out * (filled > 0).astype(jnp.float32)[:, None]
        return (accum.at[row_index].add(slot_out), None)
    total, _ = lax.scan(expert_step, total, (exp_gate, exp_up, exp_down, jnp.arange(EXPERTS, dtype=jnp.int32)))
    out = (widened + total).astype(jnp.bfloat16)
    return (out, new_state)
```

```python
import functools

import jax
import jax.numpy as jnp
from jax import lax
from jax.experimental import pallas as pl
from jax.experimental.pallas import tpu as pltpu
from jax.sharding import PartitionSpec as P

HEAD_P = 64
NSTATE = 64
GROUPS = 4
HPG = 4
LANES = 128
STATE_COLS = 512


EPSILON = 1e-06


def split_bf16(value):
    high = value.astype(jnp.bfloat16)
    low = (value - high.astype(jnp.float32)).astype(jnp.bfloat16)
    return high, low


def state_kernel(scaled_ref, decay_ref, input_ref, read_ref, state_ref, new_ref, readout_ref):
    step = pl.program_id(0)
    cols = state_ref.shape[1]
    channels = scaled_ref.shape[1]
    repeats = cols // LANES
    first = step * (cols // NSTATE)
    spread = (
        lax.broadcasted_iota(jnp.int32, (channels, cols), 0)
        == first + lax.broadcasted_iota(jnp.int32, (channels, cols), 1) // NSTATE
    )
    spread = spread.astype(jnp.float32).astype(jnp.bfloat16)
    collect = (
        lax.broadcasted_iota(jnp.int32, (cols, channels), 1)
        == first + lax.broadcasted_iota(jnp.int32, (cols, channels), 0) // NSTATE
    )
    collect = collect.astype(jnp.float32).astype(jnp.bfloat16)
    dot = functools.partial(jnp.dot, preferred_element_type=jnp.float32)
    high, low = split_bf16(scaled_ref[...])
    x_cols = dot(high, spread) + dot(low, spread)
    wide = lambda ref: jnp.concatenate([ref[...]] * repeats, axis=1)
    new = wide(decay_ref) * state_ref[...] + x_cols * wide(input_ref)
    new_ref[...] = new
    high, low = split_bf16(new * wide(read_ref))
    part = dot(high, collect) + dot(low, collect)

    @pl.when(step == 0)
    def _():
        readout_ref[...] = part

    @pl.when(step > 0)
    def _():
        readout_ref[...] += part


def run_state(scaled, decay, inputs, reads, state):
    rows, width = state.shape
    cols = min(STATE_COLS, width)
    whole = lambda shape: pl.BlockSpec(shape, lambda j: (0, 0))
    block = pl.BlockSpec((rows, cols), lambda j: (0, j))
    return pl.pallas_call(
        state_kernel,
        grid=(width // cols,),
        in_specs=[whole(scaled.shape), whole(decay.shape), whole(inputs.shape), whole(reads.shape), block],
        out_specs=[block, whole(scaled.shape)],
        out_shape=[
            jax.ShapeDtypeStruct(state.shape, jnp.float32),
            jax.ShapeDtypeStruct(scaled.shape, jnp.float32),
        ],
    )(scaled, decay, inputs, reads, state)


def state_update(
    proj_x,
    proj_z,
    proj_bc,
    proj_dt,
    tail_x,
    tail_bc,
    taps_x,
    taps_bc,
    ssm_state,
    dt_bias,
    decay_log,
    group_gain,
):
    window_x = jnp.concatenate([tail_x, proj_x[:, None]], axis=1).astype(jnp.float32)
    conv_x = jax.nn.silu(jnp.sum(window_x * taps_x.astype(jnp.float32)[None], axis=1))
    window_bc = jnp.concatenate([tail_bc, proj_bc[:, None]], axis=1).astype(jnp.float32)
    conv_bc = jax.nn.silu(jnp.sum(window_bc * taps_bc.astype(jnp.float32)[None], axis=1))
    count = proj_x.shape[0]
    heads = proj_dt.shape[1]
    x_heads = conv_x.reshape(count, heads, HEAD_P)
    grouped_bc = conv_bc.reshape(count, 2, heads // HPG, NSTATE)
    to_rows = lambda v: jnp.repeat(v, HPG, axis=1).reshape(count * heads, NSTATE)
    twice = lambda v: jnp.concatenate([v] * (LANES // NSTATE), axis=1)
    input_rows = twice(to_rows(grouped_bc[:, 0]))
    read_rows = twice(to_rows(grouped_bc[:, 1]))
    step_size = jax.nn.softplus(proj_dt.astype(jnp.float32) + dt_bias)
    decay = jnp.exp(-step_size * jnp.exp(decay_log))
    decay_rows = jnp.broadcast_to(decay[:, :, None], (count, heads, LANES)).reshape(-1, LANES)
    scaled = (step_size[:, :, None] * x_heads).reshape(count * heads, HEAD_P)
    new_state, readout = run_state(
        scaled, decay_rows, input_rows, read_rows, ssm_state.reshape(count * heads, -1)
    )
    gated = readout.reshape(count, heads * HEAD_P) * jax.nn.silu(proj_z.astype(jnp.float32))
    grouped = gated.reshape(count, heads // HPG, HPG * HEAD_P)
    grouped = grouped * lax.rsqrt(jnp.mean(grouped * grouped, axis=-1, keepdims=True) + EPSILON)
    y_out = (grouped.reshape(count, heads * HEAD_P) * group_gain).astype(jnp.bfloat16)
    return (y_out, new_state.reshape(count, heads, HEAD_P * NSTATE))


def ffn_kernel(
    x_ref, weight_ref, score_ref, dgate_ref, dup_ref, ddown_ref, egate_ref, eup_ref, edown_ref, out_ref
):
    dot = functools.partial(jnp.dot, preferred_element_type=jnp.float32)
    x = x_ref[...]
    scale = jax.nn.sigmoid(dot(x, score_ref[...]))
    dense = (scale * jax.nn.silu(dot(x, dgate_ref[...])) * dot(x, dup_ref[...])).astype(jnp.bfloat16)
    expert = weight_ref[...] * jax.nn.silu(dot(x, egate_ref[...])) * dot(x, eup_ref[...])
    expert = expert.astype(jnp.bfloat16)
    out_ref[...] = (dot(dense, ddown_ref[...]) + dot(expert, edown_ref[...])).astype(jnp.bfloat16)


def run_ffn(x, weight, *weights):
    rows, width = x.shape
    block = min(rows, 256)
    whole = lambda v: pl.BlockSpec(v.shape, lambda i: (0, 0))
    part = lambda cols: pl.BlockSpec((block, cols), lambda i: (i, 0))
    return pl.pallas_call(
        ffn_kernel,
        grid=(rows // block,),
        in_specs=[part(width), part(1)] + [whole(v) for v in weights],
        out_specs=part(width),
        out_shape=jax.ShapeDtypeStruct((rows, width), jnp.bfloat16),
        compiler_params=pltpu.CompilerParams(vmem_limit_bytes=48 * 1024 * 1024),
    )(x, weight, *weights)


def gather_ep(value):
    count = lax.axis_size("ep")
    return lax.all_to_all(
        jnp.broadcast_to(value[None], (count,) + value.shape), "ep", 0, 0, tiled=True
    )


def swap_cores(value):
    return lax.ppermute(value, "tp", [(0, 1), (1, 0)])


def shards(
    resid,
    proj_x,
    proj_z,
    proj_bc,
    proj_dt,
    tail_x,
    tail_bc,
    taps_x,
    taps_bc,
    ssm_state,
    dt_bias,
    decay_log,
    group_gain,
    out_proj,
    ffn_gain,
    dense_gate,
    dense_up,
    dense_down,
    branch_gate,
    group_weights,
    expert_ids,
    expert_weights,
    exp_gate,
    exp_up,
    exp_down,
):
    y_out, new_state = state_update(
        proj_x,
        proj_z,
        proj_bc,
        proj_dt,
        tail_x,
        tail_bc,
        taps_x,
        taps_bc,
        ssm_state,
        dt_bias,
        decay_log,
        group_gain,
    )
    experts = lax.axis_size("ep")
    expert_own = lax.axis_index("ep")
    cores = lax.axis_size("tp")
    core = lax.axis_index("tp")
    rows_each, width = resid.shape
    half = rows_each // cores
    partial_value = jnp.dot(
        gather_ep(y_out).reshape(experts * rows_each, -1),
        out_proj,
        preferred_element_type=jnp.float32,
    ).astype(jnp.bfloat16)
    pieces = lax.all_to_all(
        partial_value.reshape(experts * cores, half, -1), ("ep", "tp"), 0, 0, tiled=True
    ).astype(jnp.float32)
    mixed = jnp.sum(pieces.reshape(experts, cores, half, -1), axis=1)
    mixed = mixed.transpose(1, 0, 2).reshape(half, width)
    own = lax.dynamic_slice_in_dim(resid, core * half, half, 0)
    resid_new = (own.astype(jnp.float32) + mixed).astype(jnp.bfloat16)
    widened = resid_new.astype(jnp.float32)
    normed = (
        widened
        * lax.rsqrt(jnp.mean(widened * widened, axis=-1, keepdims=True) + EPSILON)
        * ffn_gain
    ).astype(jnp.bfloat16)
    near = gather_ep(normed).reshape(experts * half, width)
    far = swap_cores(near)
    pick = (jnp.arange(GROUPS, dtype=jnp.int32) == expert_own // (experts // GROUPS)).astype(
        jnp.float32
    )
    coarse = jnp.sum(group_weights * pick[None], axis=1)
    fine = jnp.sum(jnp.where(expert_ids == expert_own, expert_weights, 0.0), axis=1)
    weight = (fine * coarse).reshape(experts, cores, half)
    near_weight = lax.dynamic_index_in_dim(weight, core, 1, keepdims=False).reshape(-1, 1)
    far_weight = lax.dynamic_index_in_dim(weight, 1 - core, 1, keepdims=False).reshape(-1, 1)
    score = jnp.broadcast_to(branch_gate[:, None], (width, dense_gate.shape[1]))
    weights = (score, dense_gate, dense_up, dense_down, exp_gate[0], exp_up[0], exp_down[0])
    near_part = run_ffn(near, near_weight, *weights)
    far_part = run_ffn(far, far_weight, *weights)
    both = near_part.astype(jnp.float32) + swap_cores(far_part).astype(jnp.float32)
    pieces = lax.all_to_all(
        both.astype(jnp.bfloat16).reshape(experts, half, width), "ep", 0, 0, tiled=True
    )
    branch = jnp.sum(pieces.astype(jnp.float32), axis=0)
    return ((widened + branch).astype(jnp.bfloat16), new_state)


def solution(mesh):
    return jax.shard_map(
        shards,
        mesh=mesh,
        in_specs=(
            P("ep", None),
            P("ep", "tp"),
            P("ep", "tp"),
            P("ep", None, "tp"),
            P("ep", "tp"),
            P("ep", None, "tp"),
            P("ep", None, None, "tp"),
            P(None, "tp"),
            P(None, None, "tp"),
            P("ep", "tp", None),
            P("tp"),
            P("tp"),
            P("tp"),
            P("tp", "ep"),
            P(),
            P(None, ("ep", "tp")),
            P(None, ("ep", "tp")),
            P(("ep", "tp"), None),
            P(),
            P(),
            P(),
            P(),
            P("ep", None, "tp"),
            P("ep", None, "tp"),
            P("ep", "tp", None),
        ),
        out_specs=(P(("ep", "tp"), None), P("ep", "tp", None)),
        check_vma=False,
    )
```
